1024 devices in a mesh: dp: 8 (over x), kv: 64 (over z, y), tp: 2 (over core).
Axes of the slice: x: 8, y: 8, z: 8, core: 2. Of those that a mesh axis runs over, the one named last changes fastest.
Arguments:
- tokens: bfloat16 [1024, 4096], P('dp', ('kv', 'tp')), may hold values from -7 to 7
- mix_gain: float32 [4096], replicated, may hold values from 0.1 to 1.9
- query_weight: bfloat16 [16, 128, 4096], P('tp', 'kv'), may hold values from -0.09375 to 0.09375
- forget_weight: bfloat16 [16, 128, 4096], P('tp', 'kv'), may hold values from -0.09375 to 0.09375
- value_weight: bfloat16 [16, 128, 4096], P('tp', 'kv'), may hold values from -0.09375 to 0.09375
- gate_weight: bfloat16 [16, 128, 4096], P('tp', 'kv'), may hold values from -0.09375 to 0.09375
- lower_bound: float32 [16, 128], P('tp'), may hold values from 0.02 to 0.9
- recurrent_state: float32 [1024, 16, 128, 128], P(('dp', 'kv'), 'tp'), may hold values from -3 to 3
- head_gain: float32 [16, 128], P('tp'), may hold values from 0.1 to 1.9
- out_weight: bfloat16 [16, 128, 4096], P(None, None, ('kv', 'tp')), may hold values from -0.125 to 0.125
- mlp_gain: float32 [4096], replicated, may hold values from 0.1 to 1.9
- up_weight: bfloat16 [4096, 16384], P(None, ('kv', 'tp')), may hold values from -0.09375 to 0.09375
- down_weight: bfloat16 [16384, 4096], P(('kv', 'tp')), may hold values from -0.1875 to 0.1875
Outputs:
- layer_output: bfloat16 [1024, 4096], P('dp', ('kv', 'tp'))
- next_state: float32 [1024, 16, 128, 128], P(('dp', 'kv'), 'tp')
The draws below stay inside these ranges and needn't reach their ends.
All inputs are finite; a program needn't handle non-finite values.
Results may differ from the reference program's by a relative error of at most 0.0072.
Values may be sent and summed in bfloat16 or wider, within the bound.
A program may use at most 32 MiB of HBM per device.

```python
import math
import jax
import jax.numpy as jnp
from jax import lax

D = 4096
HEADS = 16
KEY_DIM = 128
VALUE_DIM = 128
FF = 16384
BATCH = 1024


def draw_tokens(key, part):
    noise_key = jax.random.fold_in(jax.random.fold_in(key, 17), 0)
    column = jnp.arange(D, dtype=jnp.float32) / (D - 1)
    values = jnp.clip(jax.random.normal(noise_key, (BATCH, D), jnp.float32), -4.0, 4.0)
    spread = math.log(3.0)
    scaled = values * jnp.exp(spread * (column - 0.5))
    return scaled.astype(jnp.bfloat16)


def raised(entries, own_key, source, target, shards_of, factor):
    def block_of(axis_at):
        return (jnp.arange(entries.shape[axis_at]) // (entries.shape[axis_at] // shards_of)).reshape((-1,) + (1,) * (entries.ndim - 1 - axis_at))

    first = jax.random.permutation(own_key, shards_of)[block_of(target)]
    other_side = (block_of(target) + shards_of // 2) % shards_of
    return jnp.where((block_of(source) == first) | (block_of(source) == other_side), factor * entries, entries)


def level_of(own_key, extent, pieces, low, largest):
    loudness = 1.0
    for dim, shards_of in pieces:
        draws = jax.random.uniform(jax.random.fold_in(jax.random.fold_in(own_key, 6), dim), (shards_of,), jnp.float32, low / len(pieces), largest / len(pieces))
        loudness = loudness * jnp.repeat(jnp.exp(draws), extent[dim] // shards_of).reshape((-1,) + (1,) * (len(extent) - 1 - dim))
    return loudness


def centred(own_key, dims, deviation, limit, cuts=(), kind=jnp.bfloat16):
    level = level_of(own_key, dims, cuts, -0.22, 0.18) if cuts else 1.0
    drawn = jax.random.normal(own_key, dims, jnp.float32) * deviation * level
    return jnp.minimum(jnp.maximum(drawn, -limit), limit).astype(kind)


def gaussian_with(stream_key, dims, deviation, bound, pieces, heavy, held_as=jnp.bfloat16):
    drawn = deviation * jax.random.normal(stream_key, dims, jnp.float32)
    if pieces:
        drawn = drawn * level_of(stream_key, dims, pieces, -0.22, 0.18)
    return jnp.clip(raised(drawn, jax.random.fold_in(stream_key, 3), *heavy), -bound, bound).astype(held_as)


def setup_inputs(seed: int = 0) -> dict:
    key_of = jax.random.split(jax.random.key(seed), 14)
    return {
        "tokens": draw_tokens(jax.random.fold_in(key_of[13], 71), 0),
        "mix_gain": jnp.clip(1.0 + 0.18 * jax.random.normal(key_of[1], (D,), jnp.float32), 0.1, 1.9),
        "query_weight": centred(key_of[2], (HEADS, KEY_DIM, D), D ** -0.5, 0.09375, ((0, 2), (1, 64))),
        "forget_weight": centred(key_of[3], (HEADS, KEY_DIM, D), D ** -0.5, 0.09375, ((0, 2), (1, 64))),
        "value_weight": centred(key_of[4], (HEADS, VALUE_DIM, D), D ** -0.5, 0.09375, ((0, 2), (1, 64))),
        "gate_weight": centred(key_of[5], (HEADS, VALUE_DIM, D), D ** -0.5, 0.09375, ((0, 2), (1, 64))),
        "lower_bound": jnp.clip(jnp.exp(math.log(0.9) - 3.8066625 * jax.random.uniform(key_of[6], (HEADS, KEY_DIM), jnp.float32) ** level_of(key_of[6], (HEADS, KEY_DIM), ((0, 2),), -0.2, 0.2)), 0.02, 0.9),
        "recurrent_state": centred(key_of[7], (BATCH, HEADS, KEY_DIM, VALUE_DIM), 0.5, 3.0, ((0, 512), (1, 2)), jnp.float32),
        "head_gain": jnp.clip(1.0 + 0.18 * jax.random.normal(key_of[8], (HEADS, VALUE_DIM), jnp.float32), 0.1, 1.9),
        "out_weight": centred(key_of[9], (HEADS, VALUE_DIM, D), (HEADS * VALUE_DIM) ** -0.5, 0.125, ((2, 128),)),
        "mlp_gain": jnp.clip(1.0 + 0.18 * jax.random.normal(key_of[10], (D,), jnp.float32), 0.1, 1.9),
        "up_weight": centred(key_of[11], (D, FF), D ** -0.5, 0.09375, ((1, 128),)),
        "down_weight": gaussian_with(key_of[12], (FF, D), FF ** -0.5, 0.1875, ((0, 128),), (0, 1, 128, 5.5)),
    }


epsilon = 1e-06

def rms_rows(matrix, gain_vector):
    as_float = matrix.astype(jnp.float32)
    inv_root = lax.rsqrt(lax.optimization_barrier(jnp.mean(as_float * as_float, axis=1, keepdims=True)) + epsilon)
    return (as_float * inv_root * gain_vector).astype(jnp.bfloat16)

def project_rows(normed, weight):
    flat_weight = weight.reshape(-1, weight.shape[2])
    product = lax.dot_general(normed, flat_weight, (((1,), (1,)), ((), ())), preferred_element_type=jnp.float32).astype(jnp.bfloat16)
    return product.reshape(normed.shape[0], weight.shape[0], weight.shape[1])

def reference(tokens, mix_gain, query_weight, forget_weight, value_weight, gate_weight, lower_bound, recurrent_state, head_gain, out_weight, mlp_gain, up_weight, down_weight):
    normed = rms_rows(tokens, mix_gain)
    pre_query, pre_forget, value_rows, pre_gate = lax.optimization_barrier((project_rows(normed, query_weight), project_rows(normed, forget_weight), project_rows(normed, value_weight), project_rows(normed, gate_weight)))
    log_forget = jnp.logaddexp(jnp.log(lower_bound), jnp.log1p(-lower_bound) + jax.nn.log_sigmoid(pre_forget.astype(jnp.float32)))
    key_rows = -jnp.expm1(log_forget)
    next_state = jnp.exp(log_forget)[:, :, :, None] * recurrent_state + key_rows[:, :, :, None] * value_rows.astype(jnp.float32)[:, :, None, :]
    query_act = jax.nn.silu(pre_query.astype(jnp.float32))
    readout = jnp.einsum('bhk,bhkv->bhv', query_act, next_state, precision=lax.Precision.HIGHEST)
    inv_head = lax.rsqrt(lax.optimization_barrier(jnp.mean(readout * readout, axis=2, keepdims=True)) + epsilon)
    mixed_heads = (readout * inv_head * head_gain * jax.nn.silu(pre_gate.astype(jnp.float32))).astype(jnp.bfloat16)
    projected = jnp.dot(mixed_heads.reshape(mixed_heads.shape[0], -1), out_weight.reshape(-1, out_weight.shape[2]), preferred_element_type=jnp.float32)
    residual = lax.optimization_barrier((tokens.astype(jnp.float32) + projected).astype(jnp.bfloat16))
    normed_mlp = rms_rows(residual, mlp_gain)
    hidden = jnp.square(jax.nn.relu(jnp.dot(normed_mlp, up_weight, preferred_element_type=jnp.float32))).astype(jnp.bfloat16)
    layer_output = (residual.astype(jnp.float32) + jnp.dot(hidden, down_weight, preferred_element_type=jnp.float32)).astype(jnp.bfloat16)
    return (layer_output, next_state)
```

```python
import jax
import jax.numpy as jnp
from jax import lax
from jax.experimental import pallas as pl
from jax.experimental.pallas import tpu as pltpu
from jax.sharding import Mesh
from jax.sharding import PartitionSpec as P

KV_TP = ("kv_0", "kv_1", "tp")
KV = ("kv_0", "kv_1")
DP_KV = ("dp", "kv_0", "kv_1")
MESH = pl.DeviceIdType.MESH
F32 = jnp.float32
BF16 = jnp.bfloat16
EPS = 1e-06
FAR = (4, 3, 5, 2, 6, 1, 7)
NEAR = (1, 7, 2, 6, 3, 5, 4)


class Place:
    def __init__(self):
        self.x, self.z, self.y, self.tp = (lax.axis_index(n) for n in ("dp", "kv_0", "kv_1", "tp"))
        self.other = 1 - self.tp
        self.partner = (self.x, self.z, self.y, self.other)
        self.a = self.y * self.other + self.z * self.tp
        self.b = self.z * self.other + self.y * self.tp

    def device(self, d, e):
        z = lax.rem(self.z + d * self.tp + e * self.other, 8)
        y = lax.rem(self.y + d * self.other + e * self.tp, 8)
        return (self.x, z, y, self.tp)

    def kv(self, d, e):
        _, z, y, _ = self.device(d, e)
        return z * 8 + y

    def ab(self, d, e):
        return lax.rem(self.a + d, 8), lax.rem(self.b + e, 8)


def kv_of(tp, a, b):
    return (1 - tp) * (b * 8 + a) + tp * (a * 8 + b)


def remote(src, dst, send, recv, device):
    return pltpu.make_async_remote_copy(src, dst, send, recv, device_id=device, device_id_type=MESH)


def landed(ref, sem):
    pltpu.make_async_copy(ref, ref, sem).wait()


def dot(a, b, ca, cb):
    return lax.dot_general(a, b, (((ca,), (cb,)), ((), ())), preferred_element_type=F32)


def gather_first(me, own, block, sems):
    sa, ra, sb, rb = sems
    for d in FAR:
        remote(own, block(0, 0), sa, ra.at[d], me.device(d, 0)).start()
    for e in FAR:
        remote(own, block(0, 0), sb, rb.at[e], me.device(0, e)).start()


def gather_second(me, own, block, sems):
    sa, ra, sb, rb = sems
    for d in NEAR:
        landed(own, ra.at[d])
        for e in FAR:
            remote(block(d, 0), block(d, 0), sb, rb.at[e], me.device(0, e)).start()


def gather_drain(own, row, sems):
    sa, ra, sb, rb = sems
    for _ in range(7):
        landed(own, sa)
        landed(row, sb)


def column_mask(shape, lo, hi):
    lane = lax.broadcasted_iota(jnp.int32, shape, 1)
    return (lane >= lo) & (lane < hi)


def squeezed_lanes(tile_of, tp, b, half):
    result = None
    for i in range(4):
        kv = kv_of(tp, half * 4 + i, b)
        tile, off = kv // 2, lax.rem(kv, 2) * 64 + tp * 32
        v = pltpu.roll(tile_of(tile), lax.rem(i * 32 + 128 - off, 128), 1)
        result = v if result is None else jnp.where(column_mask(v.shape, i * 32, i * 32 + 32), v, result)
    return result


def kernel(
    x_h, mg_h, q_h, f_h, v_h, g_h, lb_h, st_h, hg_h, ow_h, lg_h, up_h, dn_h,
    out_ref, nst_h,
    xv, mg, lg, lb, hg, wraw, upr, dnr, owr, st, nst,
    X, R, D, W2o, W2p, UTs, UTp, DTs, DTp, OWp,
    px1, pr1, px2, pr2, px3, pr3,
    tr, S, B, lbs, msk, O, msg, res, Y, R1, T, R2, wt,
    hs, sa1, ra1, sb1, rb1, sa2, ra2, sb2, rb2, sa3, ra3, sb3, rb3,
    s_a2a, r_a2a, s1, r1, s2, r2, sd, rd, so,
):
    me = Place()
    tp, other = me.tp, me.other

    bar = pltpu.get_barrier_semaphore()
    for d in range(1, 8):
        pl.semaphore_signal(bar, inc=1, device_id=me.device(d, 0), device_id_type=MESH)
        pl.semaphore_signal(bar, inc=1, device_id=me.device(0, d), device_id_type=MESH)
    pl.semaphore_signal(bar, inc=1, device_id=me.partner, device_id_type=MESH)

    loads = []

    def load(src, dst, k):
        cp = pltpu.make_async_copy(src, dst, hs.at[k])
        cp.start()
        return cp

    l_x = load(x_h, xv, 0)
    l_mg = load(mg_h, mg, 1)
    for kind, w in enumerate((q_h, f_h, v_h, g_h)):
        for h in range(8):
            pltpu.make_async_copy(w.at[h], wraw.at[pl.ds(kind * 16 + h * 2, 2)], hs.at[2]).start()
    l_lg = load(lg_h, lg, 3)
    l_lb = load(lb_h, lb, 4)
    l_hg = load(hg_h, hg, 5)
    l_ow = load(ow_h, owr, 6)
    l_st = load(st_h, st, 7)
    l_up = load(up_h, upr, 8)
    l_dn = load(dn_h, dnr, 9)

    l_mg.wait()
    landed(wraw, hs.at[2])

    def prep_w(i, _):
        b, half = i // 2, lax.rem(i, 2)

        def tile_of(t):
            w = wraw[:, pl.ds(pl.multiple_of(t * 128, 128), 128)].astype(F32)
            return w * mg[pl.ds(t, 1), :]

        W2o[b, half] = squeezed_lanes(tile_of, tp, b, half).astype(BF16)
        wt[b, half] = squeezed_lanes(tile_of, other, b, half).astype(BF16)
        return 0

    lax.fori_loop(0, 16, prep_w, 0)
    l_x.wait()
    l_ow.wait()

    pl.semaphore_wait(bar, 15)

    def x_block(d, e):
        a, b = me.ab(8 - d, 8 - e)
        return X.at[b, a]

    sems1 = (sa1, ra1, sb1, rb1)
    gather_first(me, xv, x_block, sems1)
    X[me.b, me.a] = xv[...]
    remote(wt, W2p, sd.at[0], rd.at[0], me.partner).start()
    remote(owr.at[pl.ds(other * 8, 8)], OWp, sd.at[1], rd.at[1], me.partner).start()
    gather_second(me, xv, x_block, sems1)

    landed(W2p, rd.at[0])

    def mm1(e, acc, sq):
        b = lax.rem(me.b + 8 - e, 8)
        xr = X[b].reshape(256, 128)
        xf = xr.astype(F32)
        sq = sq + jnp.sum(xf * xf, axis=0, keepdims=True)
        for half in range(2):
            w = jnp.concatenate([W2o[b, half], W2p[b, half]], axis=0)
            acc = acc + dot(w, xr[half * 128 : half * 128 + 128], 1, 0)
        return acc, sq

    acc, sq = jnp.zeros((128, 128), F32), jnp.zeros((1, 128), F32)
    for e in (0,) + NEAR:
        if e:
            landed(X.at[0], rb1.at[e])
        acc, sq = mm1(e, acc, sq)
    px1[0:64] = acc[64:128]
    px1[64:72] = jnp.broadcast_to(sq, (8, 128))
    remote(px1, pr1, sd.at[2], rd.at[2], me.partner).start()
    landed(pr1, rd.at[2])
    inv = lax.rsqrt((sq + pr1[64:65]) * (1.0 / 4096.0) + EPS)
    pre = ((acc[0:64] + pr1[0:64]) * inv).astype(BF16).astype(F32)
    tr[...] = pre.T
    S[...] = jnp.concatenate([tr[pl.ds(0, 64, stride=2), :], tr[pl.ds(1, 64, stride=2), :]], axis=1)

    mine = me.kv(0, 0)
    order = sorted(
        ((d, e) for d in range(8) for e in range(8) if d or e),
        key=lambda t: -(min(t[0], 8 - t[0]) + min(t[1], 8 - t[1])),
    )
    for d, e in order:
        k = me.kv(d, e)
        remote(S.at[pl.ds(k, 1)], B.at[pl.ds(mine, 1)], s_a2a, r_a2a, me.device(d, e)).start()
    B[pl.ds(mine, 1), :] = S[pl.ds(mine, 1), :]

    l_lb.wait()
    lane = lax.broadcasted_iota(jnp.int32, (8, 128), 1)
    head = lax.broadcasted_iota(jnp.int32, (8, 128), 0)
    sel = (lax.rem(lane, 64) // 2 == 8 + head).astype(F32)
    lbs[...] = lax.dot_general(
        lb[...], sel, (((0,), (0,)), ((), ())), precision=lax.Precision.HIGHEST, preferred_element_type=F32
    )
    odd = lax.rem(lax.broadcasted_iota(jnp.int32, (64, 128), 1), 2)
    low = jnp.where(odd == 0, lbs[pl.ds(0, 64, stride=2), :], lbs[pl.ds(1, 64, stride=2), :])
    l_lg.wait()
    l_up.wait()

    def prep_up(i, _):
        b, half = i // 2, lax.rem(i, 2)
        for core in range(2):
            rows = [upr[kv_of(core, half * 4 + j, b), core] for j in range(4)]
            u = jnp.concatenate(rows, axis=0).astype(F32).T
            g = squeezed_lanes(lambda t: lg[pl.ds(t, 1), :], core, b, half)
            UTs[core, b, half] = (u * g).astype(BF16)
        return 0

    lax.fori_loop(0, 16, prep_up, 0)
    remote(UTs.at[other], UTp, sd.at[3], rd.at[3], me.partner).start()

    l_st.wait()
    l_hg.wait()
    landed(B.at[pl.ds(0, 63)], r_a2a)
    Bv = B[...]
    ex = jnp.exp(-jnp.abs(Bv))
    big = 1.0 / (1.0 + ex)
    small = ex * big
    sig = jnp.where(Bv >= 0, big, small)
    sig_neg = jnp.where(Bv >= 0, small, big)
    decay = low + (1.0 - low) * sig
    key = (1.0 - low) * sig_neg
    act = Bv * sig
    Bb = Bv.astype(BF16)
    src = lax.broadcasted_iota(jnp.int32, (64, 128), 0)
    col = lax.broadcasted_iota(jnp.int32, (64, 128), 1)
    zero = jnp.zeros_like(Bb)
    spread = dot(jnp.where(odd == 0, Bb, zero), (col == 2 * src).astype(BF16), 0, 0)
    spread = spread + dot(jnp.where(odd == 1, Bb, zero), (col == 2 * src + 1).astype(BF16), 0, 0)
    msk[...] = spread
    vg = msk[pl.ds(0, 64, stride=2), :] + msk[pl.ds(1, 64, stride=2), :]
    for tok in range(2):
        for h in range(8):
            total = None
            vrow = vg[tok * 32 + 16 + h : tok * 32 + 17 + h]
            for j in range(2):
                c = tok * 64 + 2 * h + j
                old = st[tok, h, pl.ds(j, 64, stride=2), :]
                new = decay[:, c + 16 : c + 17] * old + key[:, c + 16 : c + 17] * vrow
                nst[tok, h, pl.ds(j, 64, stride=2), :] = new
                part = act[:, c : c + 1] * new
                total = part if total is None else total + part
            O[tok, h : h + 1, :] = jnp.sum(total, axis=0, keepdims=True)
    pltpu.make_async_copy(nst, nst_h, so).start()
    mixed = []
    for tok in range(2):
        o = O[tok]
        gate = vg[tok * 32 + 24 : tok * 32 + 32]
        ge = jnp.exp(-jnp.abs(gate))
        gs = jnp.where(gate >= 0, 1.0, ge) / (1.0 + ge)
        inv_head = lax.rsqrt(jnp.mean(o * o, axis=1, keepdims=True) + EPS)
        mixed.append(o * inv_head * hg[...] * (gate * gs))
    msg[...] = jnp.stack(mixed, axis=1).astype(BF16)

    def d_block(d, e):
        return D.at[:, me.kv(8 - d, 8 - e)]

    sems2 = (sa2, ra2, sb2, rb2)
    gather_first(me, msg, d_block, sems2)
    D[:, mine] = msg[...]
    gather_second(me, msg, d_block, sems2)

    l_dn.wait()

    def prep_dn(r, _):
        t = dnr[:, pl.ds(pl.multiple_of(r * 128, 128), 128)].astype(F32).T.astype(BF16)
        DTs[0, 2 * r] = t[0:32]
        DTs[1, 2 * r] = t[32:64]
        DTs[0, 2 * r + 1] = t[64:96]
        DTs[1, 2 * r + 1] = t[96:128]
        return 0

    lax.fori_loop(0, 32, prep_dn, 0)
    remote(DTs.at[other], DTp, sd.at[4], rd.at[4], me.partner).start()

    landed(OWp, rd.at[1])
    for e in NEAR:
        landed(D.at[:, pl.ds(0, 8)], rb2.at[e])
    heads = D.reshape(8, 128, 128)
    acc2 = jnp.zeros((64, 128), F32)
    for h in range(8):
        w = jnp.concatenate([owr[tp * 8 + h], OWp[h]], axis=0)
        acc2 = acc2 + dot(w, heads[h], 1, 1)
    px2[...] = acc2[32:64]
    remote(px2, pr2, sd.at[5], rd.at[5], me.partner).start()
    landed(pr2, rd.at[5])
    res[...] = (xv[...].astype(F32) + acc2[0:32] + pr2[...]).astype(BF16)

    def r_block(d, e):
        a, b = me.ab(8 - d, 8 - e)
        return R.at[b, a]

    sems3 = (sa3, ra3, sb3, rb3)
    gather_first(me, res, r_block, sems3)
    R[me.b, me.a] = res[...]
    gather_second(me, res, r_block, sems3)

    landed(UTp, rd.at[3])

    def mm3(e, acc, sq):
        b = lax.rem(me.b + 8 - e, 8)
        xr = R[b].reshape(256, 128)
        xf = xr.astype(F32)
        sq = sq + jnp.sum(xf * xf, axis=0, keepdims=True)
        for half in range(2):
            w = jnp.concatenate([UTs[tp, b, half], UTp[b, half]], axis=0)
            acc = acc + dot(w, xr[half * 128 : half * 128 + 128], 1, 0)
        return acc, sq

    acc3, sq3 = jnp.zeros((256, 128), F32), jnp.zeros((1, 128), F32)
    for e in (0,) + NEAR:
        if e:
            landed(R.at[0], rb3.at[e])
        acc3, sq3 = mm3(e, acc3, sq3)
    px3[0:256] = acc3
    px3[256:264] = jnp.broadcast_to(sq3, (8, 128))
    remote(px3, pr3, sd.at[6], rd.at[6], me.partner).start()
    landed(pr3, rd.at[6])
    inv3 = lax.rsqrt((sq3 + pr3[256:257]) * (1.0 / 4096.0) + EPS)
    pre3 = jnp.concatenate([acc3[0:128] + pr3[128:256], acc3[128:256] + pr3[0:128]], axis=0)
    act3 = jnp.maximum(pre3 * inv3, 0.0)
    hidden = (act3 * act3).astype(BF16)

    landed(DTp, rd.at[4])
    first = None
    for d in FAR + (0,):
        rows = []
        for e in range(8):
            k = me.kv(d, e)
            rows.append(jnp.concatenate([DTs[tp, k], DTp[k]], axis=1))
        y = dot(jnp.concatenate(rows, axis=0), hidden, 1, 0)
        Y[d, 0] = y[0:32]
        Yb = y.astype(BF16)
        for e in range(1, 8):
            T[d, e] = Yb[e * 32 : e * 32 + 32]
        for e in FAR:
            remote(T.at[d, e], R1.at[d, e], s1, r1.at[d], me.device(0, e)).start()
    for d in FAR + (0,):
        landed(R1.at[0, pl.ds(0, 7)], r1.at[d])
        t = Y[d, 0]
        for e in range(1, 8):
            t = t + R1[d, e].astype(F32)
        if d:
            T[d, 0] = t.astype(BF16)
            remote(T.at[d, 0], R2.at[d], s2, r2.at[d], me.device(d, 0)).start()
        else:
            first = t
    total = res[...].astype(F32) + first
    for d in NEAR:
        landed(R2.at[d], r2.at[d])
        total = total + R2[d].astype(F32)
    out_ref[...] = total.astype(BF16)

    gather_drain(xv, X.at[0], sems1)
    gather_drain(msg, D.at[:, pl.ds(0, 8)], sems2)
    gather_drain(res, R.at[0], sems3)
    landed(B.at[pl.ds(0, 63)], s_a2a)
    for d in range(8):
        landed(R1.at[0, pl.ds(0, 7)], s1)
    landed(R2.at[pl.ds(0, 7)], s2)
    landed(wt, sd.at[0])
    landed(OWp, sd.at[1])
    landed(px1, sd.at[2])
    landed(UTp, sd.at[3])
    landed(DTp, sd.at[4])
    landed(px2, sd.at[5])
    landed(px3, sd.at[6])
    pltpu.make_async_copy(nst, nst_h, so).wait()


def local(tokens, mix_gain, q, f, v, g, lower, state, head_gain, out_w, mlp_gain, up, down):
    dma = pltpu.SemaphoreType.DMA
    gather_sems = [dma, dma((8,)), dma, dma((8,))]
    vm = pltpu.VMEM
    out, nst = pl.pallas_call(
        kernel,
        out_shape=(jax.ShapeDtypeStruct((32, 128), BF16), jax.ShapeDtypeStruct(state.shape, F32)),
        in_specs=[pl.BlockSpec(memory_space=pltpu.HBM)] * 13,
        out_specs=(pl.BlockSpec(memory_space=pltpu.VMEM), pl.BlockSpec(memory_space=pltpu.HBM)),
        scratch_shapes=[
            vm((32, 128), BF16), vm((32, 128), F32), vm((32, 128), F32), vm((8, 128), F32), vm((8, 128), F32),
            vm((64, 4096), BF16), vm((64, 2, 32, 128), BF16), vm((128, 4096), BF16), vm((16, 32, 128), BF16),
            vm((2, 8, 128, 128), F32), vm((2, 8, 128, 128), F32),
            vm((8, 8, 32, 128), BF16), vm((8, 8, 32, 128), BF16), vm((8, 64, 2, 128), BF16),
            vm((8, 2, 64, 128), BF16), vm((8, 2, 64, 128), BF16),
            vm((2, 8, 2, 128, 128), BF16), vm((8, 2, 128, 128), BF16),
            vm((2, 64, 32, 128), BF16), vm((64, 32, 128), BF16), vm((8, 32, 128), BF16),
            vm((72, 128), F32), vm((72, 128), F32), vm((32, 128), F32), vm((32, 128), F32),
            vm((264, 128), F32), vm((264, 128), F32),
            vm((128, 64), F32), vm((64, 128), F32), vm((64, 128), F32), vm((128, 128), F32), vm((128, 128), F32),
            vm((2, 8, 128), F32), vm((8, 2, 128), BF16), vm((32, 128), BF16),
            vm((8, 1, 32, 128), F32), vm((8, 8, 32, 128), BF16), vm((8, 8, 32, 128), BF16), vm((8, 32, 128), BF16),
            vm((8, 2, 64, 128), BF16),
            dma((10,)), *gather_sems, *gather_sems, *gather_sems,
            dma, dma, dma, dma((8,)), dma, dma((8,)), dma((7,)), dma((7,)), dma,
        ],
        compiler_params=pltpu.CompilerParams(collective_id=0, has_side_effects=True, vmem_limit_bytes=60 * 1024 * 1024),
    )(
        tokens.T, mix_gain.reshape(32, 128), q, f, v, g, lower, state, head_gain,
        out_w.transpose(0, 2, 1), mlp_gain.reshape(32, 128), up.reshape(64, 2, 32, 128), down,
    )
    return (out.T, nst)


def solution(mesh):
    torus = Mesh(
        mesh.devices.reshape(mesh.shape["dp"], 8, 8, mesh.shape["tp"]), ("dp", "kv_0", "kv_1", "tp")
    )
    return jax.shard_map(
        local,
        mesh=torus,
        in_specs=(
            P("dp", KV_TP), P(), P("tp", KV, None), P("tp", KV, None), P("tp", KV, None), P("tp", KV, None),
            P("tp", None), P(DP_KV, "tp", None, None), P("tp", None), P(None, None, KV_TP), P(),
            P(None, KV_TP), P(KV_TP, None),
        ),
        out_specs=(P("dp", KV_TP), P(DP_KV, "tp", None, None)),
        check_vma=False,
    )
```

```python
import jax
import jax.numpy as jnp
from jax import lax
from jax.experimental import pallas as pl
from jax.experimental.pallas import tpu as pltpu
from jax.sharding import Mesh
from jax.sharding import PartitionSpec as P

KV_TP = ("kv_0", "kv_1", "tp")
KV = ("kv_0", "kv_1")
DP_KV = ("dp", "kv_0", "kv_1")
MESH = pl.DeviceIdType.MESH
F32 = jnp.float32
BF16 = jnp.bfloat16
EPS = 1e-06
FAR = (4, 3, 5, 2, 6, 1, 7)
NEAR = (1, 7, 2, 6, 3, 5, 4)


class Place:
    def __init__(self):
        self.x, self.z, self.y, self.tp = (lax.axis_index(n) for n in ("dp", "kv_0", "kv_1", "tp"))
        self.other = 1 - self.tp
        self.partner = (self.x, self.z, self.y, self.other)
        self.a = self.y * self.other + self.z * self.tp
        self.b = self.z * self.other + self.y * self.tp

    def device(self, d, e):
        z = lax.rem(self.z + d * self.tp + e * self.other, 8)
        y = lax.rem(self.y + d * self.other + e * self.tp, 8)
        return (self.x, z, y, self.tp)

    def kv(self, d, e):
        _, z, y, _ = self.device(d, e)
        return z * 8 + y

    def ab(self, d, e):
        return lax.rem(self.a + d, 8), lax.rem(self.b + e, 8)


def kv_of(tp, a, b):
    return (1 - tp) * (b * 8 + a) + tp * (a * 8 + b)


def remote(src, dst, send, recv, device):
    return pltpu.make_async_remote_copy(src, dst, send, recv, device_id=device, device_id_type=MESH)


def landed(ref, sem):
    pltpu.make_async_copy(ref, ref, sem).wait()


def dot(a, b, ca, cb):
    return lax.dot_general(a, b, (((ca,), (cb,)), ((), ())), preferred_element_type=F32)


def gather_first(me, own, block, sems):
    sa, ra, sb, rb = sems
    for d in FAR:
        remote(own, block(0, 0), sa, ra.at[d], me.device(d, 0)).start()
    for e in FAR:
        remote(own, block(0, 0), sb, rb.at[e], me.device(0, e)).start()


def gather_second(me, own, block, sems):
    sa, ra, sb, rb = sems
    for d in NEAR:
        landed(own, ra.at[d])
        for e in FAR:
            remote(block(d, 0), block(d, 0), sb, rb.at[e], me.device(0, e)).start()


def gather_drain(own, row, sems):
    sa, ra, sb, rb = sems
    for _ in range(7):
        landed(own, sa)
        landed(row, sb)


def column_mask(shape, lo, hi):
    lane = lax.broadcasted_iota(jnp.int32, shape, 1)
    return (lane >= lo) & (lane < hi)


def squeezed_lanes(tile_of, tp, b, half):
    result = None
    for i in range(4):
        kv = kv_of(tp, half * 4 + i, b)
        tile, off = kv // 2, lax.rem(kv, 2) * 64 + tp * 32
        v = pltpu.roll(tile_of(tile), lax.rem(i * 32 + 128 - off, 128), 1)
        result = v if result is None else jnp.where(column_mask(v.shape, i * 32, i * 32 + 32), v, result)
    return result


def kernel(
    x_h, mg_h, q_h, f_h, v_h, g_h, lb_h, st_h, hg_h, ow_h, lg_h, up_h, dn_h,
    out_ref, nst,
    xv, mg, lg, lb, hg, wraw, upr, dnr, owr, st,
    X, R, D, W2o, W2p, UTs, UTp, DTs, DTp, OWp,
    px1, pr1, px2, pr2, px3, pr3,
    tr, S, B, lbs, msk, O, msg, res, Y, R1, T, R2, wt,
    hs, sa1, ra1, sb1, rb1, sa2, ra2, sb2, rb2, sa3, ra3, sb3, rb3,
    s_a2a, r_a2a, s1, r1, s2, r2, sd, rd, so,
):
    me = Place()
    tp, other = me.tp, me.other

    bar = pltpu.get_barrier_semaphore()
    for d in range(1, 8):
        pl.semaphore_signal(bar, inc=1, device_id=me.device(d, 0), device_id_type=MESH)
        pl.semaphore_signal(bar, inc=1, device_id=me.device(0, d), device_id_type=MESH)
    pl.semaphore_signal(bar, inc=1, device_id=me.partner, device_id_type=MESH)

    loads = []

    def load(src, dst, k):
        cp = pltpu.make_async_copy(src, dst, hs.at[k])
        cp.start()
        return cp

    l_x = load(x_h, xv, 0)
    l_mg = load(mg_h, mg, 1)
    for kind, w in enumerate((q_h, f_h, v_h, g_h)):
        for h in range(8):
            pltpu.make_async_copy(w.at[h], wraw.at[pl.ds(kind * 16 + h * 2, 2)], hs.at[2]).start()
    l_lg = load(lg_h, lg, 3)
    l_lb = load(lb_h, lb, 4)
    l_hg = load(hg_h, hg, 5)
    l_ow = load(ow_h, owr, 6)
    l_st = load(st_h, st, 7)
    l_up = load(up_h, upr, 8)
    l_dn = load(dn_h, dnr, 9)

    l_mg.wait()
    landed(wraw, hs.at[2])

    def prep_w(i, _):
        b, half = i // 2, lax.rem(i, 2)

        def tile_of(t):
            w = wraw[:, pl.ds(pl.multiple_of(t * 128, 128), 128)].astype(F32)
            return w * mg[pl.ds(t, 1), :]

        W2o[b, half] = squeezed_lanes(tile_of, tp, b, half).astype(BF16)
        wt[b, half] = squeezed_lanes(tile_of, other, b, half).astype(BF16)
        return 0

    lax.fori_loop(0, 16, prep_w, 0)
    l_x.wait()
    l_ow.wait()

    pl.semaphore_wait(bar, 15)

    def x_block(d, e):
        a, b = me.ab(8 - d, 8 - e)
        return X.at[b, a]

    sems1 = (sa1, ra1, sb1, rb1)
    gather_first(me, xv, x_block, sems1)
    X[me.b, me.a] = xv[...]
    remote(wt, W2p, sd.at[0], rd.at[0], me.partner).start()
    remote(owr.at[pl.ds(other * 8, 8)], OWp, sd.at[1], rd.at[1], me.partner).start()
    gather_second(me, xv, x_block, sems1)

    landed(W2p, rd.at[0])

    def mm1(e, acc, sq):
        b = lax.rem(me.b + 8 - e, 8)
        xr = X[b].reshape(256, 128)
        xf = xr.astype(F32)
        sq = sq + jnp.sum(xf * xf, axis=0, keepdims=True)
        for half in range(2):
            w = jnp.concatenate([W2o[b, half], W2p[b, half]], axis=0)
            acc = acc + dot(w, xr[half * 128 : half * 128 + 128], 1, 0)
        return acc, sq

    acc, sq = jnp.zeros((128, 128), F32), jnp.zeros((1, 128), F32)
    for e in (0,) + NEAR:
        if e:
            landed(X.at[0], rb1.at[e])
        acc, sq = mm1(e, acc, sq)
    px1[0:64] = acc[64:128]
    px1[64:72] = jnp.broadcast_to(sq, (8, 128))
    remote(px1, pr1, sd.at[2], rd.at[2], me.partner).start()
    landed(pr1, rd.at[2])
    inv = lax.rsqrt((sq + pr1[64:65]) * (1.0 / 4096.0) + EPS)
    pre = ((acc[0:64] + pr1[0:64]) * inv).astype(BF16).astype(F32)
    tr[...] = pre.T
    S[...] = jnp.concatenate([tr[pl.ds(0, 64, stride=2), :], tr[pl.ds(1, 64, stride=2), :]], axis=1)

    mine = me.kv(0, 0)
    order = sorted(
        ((d, e) for d in range(8) for e in range(8) if d or e),
        key=lambda t: -(min(t[0], 8 - t[0]) + min(t[1], 8 - t[1])),
    )
    for d, e in order:
        k = me.kv(d, e)
        remote(S.at[pl.ds(k, 1)], B.at[pl.ds(mine, 1)], s_a2a, r_a2a, me.device(d, e)).start()
    B[pl.ds(mine, 1), :] = S[pl.ds(mine, 1), :]

    l_lb.wait()
    lane = lax.broadcasted_iota(jnp.int32, (8, 128), 1)
    head = lax.broadcasted_iota(jnp.int32, (8, 128), 0)
    sel = (lax.rem(lane, 64) // 2 == 8 + head).astype(F32)
    lbs[...] = lax.dot_general(
        lb[...], sel, (((0,), (0,)), ((), ())), precision=lax.Precision.HIGHEST, preferred_element_type=F32
    )
    odd = lax.rem(lax.broadcasted_iota(jnp.int32, (64, 128), 1), 2)
    low = jnp.where(odd == 0, lbs[pl.ds(0, 64, stride=2), :], lbs[pl.ds(1, 64, stride=2), :])
    l_lg.wait()
    l_up.wait()

    def prep_up(i, _):
        b, half = i // 2, lax.rem(i, 2)
        for core in range(2):
            rows = [upr[kv_of(core, half * 4 + j, b), core] for j in range(4)]
            u = jnp.concatenate(rows, axis=0).astype(F32).T
            g = squeezed_lanes(lambda t: lg[pl.ds(t, 1), :], core, b, half)
            UTs[core, b, half] = (u * g).astype(BF16)
        return 0

    lax.fori_loop(0, 16, prep_up, 0)
    remote(UTs.at[other], UTp, sd.at[3], rd.at[3], me.partner).start()

    l_st.wait()
    l_hg.wait()
    landed(B.at[pl.ds(0, 63)], r_a2a)
    Bv = B[...]
    ex = jnp.exp(-jnp.abs(Bv))
    big = 1.0 / (1.0 + ex)
    small = ex * big
    sig = jnp.where(Bv >= 0, big, small)
    sig_neg = jnp.where(Bv >= 0, small, big)
    decay = low + (1.0 - low) * sig
    key = (1.0 - low) * sig_neg
    act = Bv * sig
    Bb = Bv.astype(BF16)
    src = lax.broadcasted_iota(jnp.int32, (64, 128), 0)
    col = lax.broadcasted_iota(jnp.int32, (64, 128), 1)
    zero = jnp.zeros_like(Bb)
    spread = dot(jnp.where(odd == 0, Bb, zero), (col == 2 * src).astype(BF16), 0, 0)
    spread = spread + dot(jnp.where(odd == 1, Bb, zero), (col == 2 * src + 1).astype(BF16), 0, 0)
    msk[...] = spread
    vg = msk[pl.ds(0, 64, stride=2), :] + msk[pl.ds(1, 64, stride=2), :]
    for tok in range(2):
        for h in range(8):
            total = None
            vrow = vg[tok * 32 + 16 + h : tok * 32 + 17 + h]
            for j in range(2):
                c = tok * 64 + 2 * h + j
                old = st[tok, h, pl.ds(j, 64, stride=2), :]
                new = decay[:, c + 16 : c + 17] * old + key[:, c + 16 : c + 17] * vrow
                nst[tok, h, pl.ds(j, 64, stride=2), :] = new
                part = act[:, c : c + 1] * new
                total = part if total is None else total + part
            O[tok, h : h + 1, :] = jnp.sum(total, axis=0, keepdims=True)
    mixed = []
    for tok in range(2):
        o = O[tok]
        gate = vg[tok * 32 + 24 : tok * 32 + 32]
        ge = jnp.exp(-jnp.abs(gate))
        gs = jnp.where(gate >= 0, 1.0, ge) / (1.0 + ge)
        inv_head = lax.rsqrt(jnp.mean(o * o, axis=1, keepdims=True) + EPS)
        mixed.append(o * inv_head * hg[...] * (gate * gs))
    msg[...] = jnp.stack(mixed, axis=1).astype(BF16)

    def d_block(d, e):
        return D.at[:, me.kv(8 - d, 8 - e)]

    sems2 = (sa2, ra2, sb2, rb2)
    gather_first(me, msg, d_block, sems2)
    D[:, mine] = msg[...]
    gather_second(me, msg, d_block, sems2)

    l_dn.wait()

    def prep_dn(r, _):
        t = dnr[:, pl.ds(pl.multiple_of(r * 128, 128), 128)].astype(F32).T.astype(BF16)
        DTs[0, 2 * r] = t[0:32]
        DTs[1, 2 * r] = t[32:64]
        DTs[0, 2 * r + 1] = t[64:96]
        DTs[1, 2 * r + 1] = t[96:128]
        return 0

    lax.fori_loop(0, 32, prep_dn, 0)
    remote(DTs.at[other], DTp, sd.at[4], rd.at[4], me.partner).start()

    landed(OWp, rd.at[1])
    for e in NEAR:
        landed(D.at[:, pl.ds(0, 8)], rb2.at[e])
    heads = D.reshape(8, 128, 128)
    acc2 = jnp.zeros((64, 128), F32)
    for h in range(8):
        w = jnp.concatenate([owr[tp * 8 + h], OWp[h]], axis=0)
        acc2 = acc2 + dot(w, heads[h], 1, 1)
    px2[...] = acc2[32:64]
    remote(px2, pr2, sd.at[5], rd.at[5], me.partner).start()
    landed(pr2, rd.at[5])
    res[...] = (xv[...].astype(F32) + acc2[0:32] + pr2[...]).astype(BF16)

    def r_block(d, e):
        a, b = me.ab(8 - d, 8 - e)
        return R.at[b, a]

    sems3 = (sa3, ra3, sb3, rb3)
    gather_first(me, res, r_block, sems3)
    R[me.b, me.a] = res[...]
    gather_second(me, res, r_block, sems3)

    landed(UTp, rd.at[3])

    def mm3(e, acc, sq):
        b = lax.rem(me.b + 8 - e, 8)
        xr = R[b].reshape(256, 128)
        xf = xr.astype(F32)
        sq = sq + jnp.sum(xf * xf, axis=0, keepdims=True)
        for half in range(2):
            w = jnp.concatenate([UTs[tp, b, half], UTp[b, half]], axis=0)
            acc = acc + dot(w, xr[half * 128 : half * 128 + 128], 1, 0)
        return acc, sq

    acc3, sq3 = jnp.zeros((256, 128), F32), jnp.zeros((1, 128), F32)
    for e in (0,) + NEAR:
        if e:
            landed(R.at[0], rb3.at[e])
        acc3, sq3 = mm3(e, acc3, sq3)
    px3[0:256] = acc3
    px3[256:264] = jnp.broadcast_to(sq3, (8, 128))
    remote(px3, pr3, sd.at[6], rd.at[6], me.partner).start()
    landed(pr3, rd.at[6])
    inv3 = lax.rsqrt((sq3 + pr3[256:257]) * (1.0 / 4096.0) + EPS)
    pre3 = jnp.concatenate([acc3[0:128] + pr3[128:256], acc3[128:256] + pr3[0:128]], axis=0)
    act3 = jnp.maximum(pre3 * inv3, 0.0)
    hidden = (act3 * act3).astype(BF16)

    landed(DTp, rd.at[4])
    first = None
    for d in FAR + (0,):
        rows = []
        for e in range(8):
            k = me.kv(d, e)
            rows.append(jnp.concatenate([DTs[tp, k], DTp[k]], axis=1))
        y = dot(jnp.concatenate(rows, axis=0), hidden, 1, 0)
        Y[d, 0] = y[0:32]
        Yb = y.astype(BF16)
        for e in range(1, 8):
            T[d, e] = Yb[e * 32 : e * 32 + 32]
        for e in FAR:
            remote(T.at[d, e], R1.at[d, e], s1, r1.at[d], me.device(0, e)).start()
    for d in FAR + (0,):
        landed(R1.at[0, pl.ds(0, 7)], r1.at[d])
        t = Y[d, 0]
        for e in range(1, 8):
            t = t + R1[d, e].astype(F32)
        if d:
            T[d, 0] = t.astype(BF16)
            remote(T.at[d, 0], R2.at[d], s2, r2.at[d], me.device(d, 0)).start()
        else:
            first = t
    total = res[...].astype(F32) + first
    for d in NEAR:
        landed(R2.at[d], r2.at[d])
        total = total + R2[d].astype(F32)
    out_ref[...] = total.astype(BF16)

    gather_drain(xv, X.at[0], sems1)
    gather_drain(msg, D.at[:, pl.ds(0, 8)], sems2)
    gather_drain(res, R.at[0], sems3)
    landed(B.at[pl.ds(0, 63)], s_a2a)
    for d in range(8):
        landed(R1.at[0, pl.ds(0, 7)], s1)
    landed(R2.at[pl.ds(0, 7)], s2)
    landed(wt, sd.at[0])
    landed(OWp, sd.at[1])
    landed(px1, sd.at[2])
    landed(UTp, sd.at[3])
    landed(DTp, sd.at[4])
    landed(px2, sd.at[5])
    landed(px3, sd.at[6])


def finish(o_ref, n_ref, out, nst, s0, s1):
    a = pltpu.make_async_copy(n_ref, nst, s0)
    b = pltpu.make_async_copy(o_ref, out, s1)
    a.start()
    b.start()
    a.wait()
    b.wait()


def local(tokens, mix_gain, q, f, v, g, lower, state, head_gain, out_w, mlp_gain, up, down):
    dma = pltpu.SemaphoreType.DMA
    gather_sems = [dma, dma((8,)), dma, dma((8,))]
    vm = pltpu.VMEM
    out, nst = pl.pallas_call(
        kernel,
        out_shape=(jax.ShapeDtypeStruct((32, 128), BF16), jax.ShapeDtypeStruct(state.shape, F32)),
        in_specs=[pl.BlockSpec(memory_space=pltpu.HBM)] * 13,
        out_specs=(pl.BlockSpec(memory_space=pltpu.VMEM), pl.BlockSpec(memory_space=pltpu.VMEM)),
        scratch_shapes=[
            vm((32, 128), BF16), vm((32, 128), F32), vm((32, 128), F32), vm((8, 128), F32), vm((8, 128), F32),
            vm((64, 4096), BF16), vm((64, 2, 32, 128), BF16), vm((128, 4096), BF16), vm((16, 32, 128), BF16),
            vm((2, 8, 128, 128), F32),
            vm((8, 8, 32, 128), BF16), vm((8, 8, 32, 128), BF16), vm((8, 64, 2, 128), BF16),
            vm((8, 2, 64, 128), BF16), vm((8, 2, 64, 128), BF16),
            vm((2, 8, 2, 128, 128), BF16), vm((8, 2, 128, 128), BF16),
            vm((2, 64, 32, 128), BF16), vm((64, 32, 128), BF16), vm((8, 32, 128), BF16),
            vm((72, 128), F32), vm((72, 128), F32), vm((32, 128), F32), vm((32, 128), F32),
            vm((264, 128), F32), vm((264, 128), F32),
            vm((128, 64), F32), vm((64, 128), F32), vm((64, 128), F32), vm((128, 128), F32), vm((128, 128), F32),
            vm((2, 8, 128), F32), vm((8, 2, 128), BF16), vm((32, 128), BF16),
            vm((8, 1, 32, 128), F32), vm((8, 8, 32, 128), BF16), vm((8, 8, 32, 128), BF16), vm((8, 32, 128), BF16),
            vm((8, 2, 64, 128), BF16),
            dma((10,)), *gather_sems, *gather_sems, *gather_sems,
            dma, dma, dma, dma((8,)), dma, dma((8,)), dma((7,)), dma((7,)), dma,
        ],
        compiler_params=pltpu.CompilerParams(collective_id=0, has_side_effects=True, vmem_limit_bytes=48 * 1024 * 1024),
    )(
        *(pltpu.with_memory_space_constraint(t, pltpu.HBM) for t in (tokens.T, mix_gain.reshape(32, 128), q, f, v, g, lower, state, head_gain,
        out_w.transpose(0, 2, 1), mlp_gain.reshape(32, 128), up.reshape(64, 2, 32, 128), down,
    )))
    out, nst = pl.pallas_call(
        finish,
        out_shape=(jax.ShapeDtypeStruct((32, 128), BF16), jax.ShapeDtypeStruct(state.shape, F32)),
        in_specs=[pl.BlockSpec(memory_space=pltpu.VMEM)] * 2,
        out_specs=[pl.BlockSpec(memory_space=pltpu.HBM)] * 2,
        scratch_shapes=[dma, dma],
        compiler_params=pltpu.CompilerParams(vmem_limit_bytes=1024*1024),
    )(out, nst)
    return (out.T, nst)


def solution(mesh):
    torus = Mesh(
        mesh.devices.reshape(mesh.shape["dp"], 8, 8, mesh.shape["tp"]), ("dp", "kv_0", "kv_1", "tp")
    )
    return jax.shard_map(
        local,
        mesh=torus,
        in_specs=(
            P("dp", KV_TP), P(), P("tp", KV, None), P("tp", KV, None), P("tp", KV, None), P("tp", KV, None),
            P("tp", None), P(DP_KV, "tp", None, None), P("tp", None), P(None, None, KV_TP), P(),
            P(None, KV_TP), P(KV_TP, None),
        ),
        out_specs=(P("dp", KV_TP), P(DP_KV, "tp", None, None)),
        check_vma=False,
    )
```
